32 devices in a mesh: grp: 2 (over y), kv: 4 (over z), tp: 4 (over x, core).
Axes of the slice: x: 2, y: 2, z: 4, core: 2. Of those that a mesh axis runs over, the one named last changes fastest.
Arguments:
- tokens: bfloat16 [24, 4096], P('grp', ('kv', 'tp')), parts along dimension 0, may hold values from -70 to 70
- attn_gain: bfloat16 [4096], P('kv'), may hold values from 0.099609375 to 1.8984375
- query_weight: bfloat16 [4096, 4096], P('kv', 'tp'), may hold values from -0.09375 to 0.09375
- key_weight: bfloat16 [1024, 4096], P('tp', 'kv'), may hold values from -0.09375 to 0.09375
- value_weight: bfloat16 [1024, 4096], P('tp', 'kv'), may hold values from -0.09375 to 0.09375
- forget_weight: bfloat16 [64, 4096], P(None, 'kv'), may hold values from -0.09375 to 0.09375
- forget_bias: float32 [64], replicated, may hold values from -3 to 1
- cache_keys: bfloat16 [24, 16, 64, 4096], P('grp', 'tp', None, 'kv'), parts along dimension 0, may hold values from -620 to 620
- cache_values: bfloat16 [24, 16, 64, 4096], P('grp', 'tp', None, 'kv'), parts along dimension 0, may hold values from -6 to 6
- gate_sums: float32 [24, 64, 4096], P('grp', 'tp', 'kv'), parts along dimension 0, may hold values from -411.6 to 0
- output_weight: bfloat16 [4096, 4096], P('tp', 'kv'), may hold values from -0.09375 to 0.09375
- mixer_gain: bfloat16 [4096], P('kv'), may hold values from 0.099609375 to 1.8984375
- up_weight: bfloat16 [4096, 16384], P('kv', 'tp'), may hold values from -0.09375 to 0.09375
- down_weight: bfloat16 [16384, 4096], P('tp', 'kv'), may hold values from -0.046875 to 0.046875
Outputs:
- mixed: bfloat16 [24, 4096], P('grp', ('kv', 'tp')), parts along dimension 0
The draws below stay inside these ranges and needn't reach their ends.
There are 2 independent parts, one for each index of `grp`. The reference program is written for one: setup_inputs(seed, part) draws one part's arguments, and reference() takes and returns one part's arrays. A program takes and returns all parts, laid end to end along the dimension named above; an argument that names none is the same for every part. Nothing has to cross between parts.
All inputs are finite; a program needn't handle non-finite values.
Results may differ from the reference program's by a relative error of at most 0.008.
Values may be sent and summed in bfloat16 or wider, within the bound.
A program may use at most 64 MiB of HBM per device.

```python
import math
import jax
import jax.numpy as jnp
from jax import lax

D = 4096
QUERY_HEADS = 64
KV_HEADS = 16
HEAD_DIM = 64
FF = 16384
BATCH_SEQUENCES = 12
POS_DEV = 1024
CACHE_POSITIONS = 4096


def draw_tokens(key, part):
    base_key = jax.random.fold_in(key, 0)
    rough_key = jax.random.fold_in(key, 2)
    row_key = jax.random.fold_in(key, 3)
    columns = jnp.arange(D, dtype=jnp.float32)
    rising = jnp.exp(math.log(10.0) * (columns / D - 0.5))
    coarse_estimate = jnp.exp(jax.random.uniform(rough_key, (D,), jnp.float32, -0.35, 0.35))
    row_scale = jnp.exp(jax.random.uniform(row_key, (BATCH_SEQUENCES, 1), jnp.float32, math.log(0.3), math.log(3.0)))
    base = jnp.clip(jax.random.normal(base_key, (BATCH_SEQUENCES, D), jnp.float32), -5.0, 5.0)
    return (base * row_scale * rising * coarse_estimate).astype(jnp.bfloat16)


def draw_cache_keys(key, part):
    base_key = jax.random.fold_in(key, 0)
    shape = (BATCH_SEQUENCES, KV_HEADS, HEAD_DIM, CACHE_POSITIONS)
    base = jnp.clip(jax.random.normal(base_key, shape, jnp.float32), -5.0, 5.0)
    return base.astype(jnp.bfloat16)


def draw_gate_sums(key, part):
    key_entries = jax.random.split(key, 7)
    slow_share = 0.5
    slow = jax.random.bernoulli(key_entries[0], slow_share, (BATCH_SEQUENCES, QUERY_HEADS, 1))
    reach = jnp.exp(jax.random.uniform(key_entries[1], (BATCH_SEQUENCES, QUERY_HEADS, 1), jnp.float32, math.log(0.3), math.log(1.0))) / CACHE_POSITIONS
    fast = 1.0 / jnp.exp(jax.random.uniform(key_entries[2], (BATCH_SEQUENCES, QUERY_HEADS, 1), jnp.float32, math.log(30.0), math.log(50.0)))
    spike_probability = jnp.where(slow, reach, fast)
    blocks = CACHE_POSITIONS // POS_DEV
    block_multiplier = jnp.exp(jax.random.uniform(key_entries[3], (BATCH_SEQUENCES, QUERY_HEADS, blocks, 1), jnp.float32, math.log(0.5), math.log(2.0)))
    block_multiplier = jnp.broadcast_to(block_multiplier, (BATCH_SEQUENCES, QUERY_HEADS, blocks, POS_DEV)).reshape(BATCH_SEQUENCES, QUERY_HEADS, CACHE_POSITIONS)
    coarse_estimate = jax.random.uniform(key_entries[4], (BATCH_SEQUENCES, QUERY_HEADS, CACHE_POSITIONS), jnp.float32, 0.5, 1.5)
    position_indices = jnp.arange(CACHE_POSITIONS).reshape(1, 1, 1, CACHE_POSITIONS)
    spike_position = jax.random.randint(key_entries[5], (BATCH_SEQUENCES, QUERY_HEADS, 2, 1), 0, CACHE_POSITIONS)
    spike_magnitude = jax.random.uniform(key_entries[6], (BATCH_SEQUENCES, QUERY_HEADS, 2, 1), jnp.float32, 0.22, 0.5)
    spike_events = jnp.sum(jnp.where(position_indices == spike_position, spike_magnitude, 0.0), axis=2)
    logarithm_gate = -(spike_probability * block_multiplier * coarse_estimate + spike_events)
    suffix = jnp.flip(jnp.cumsum(jnp.flip(logarithm_gate, axis=-1), axis=-1), axis=-1) - logarithm_gate
    return suffix.astype(jnp.float32)


def block_scale(rng, extent, cuts, smallest, top_value):
    def one(dim, shards_of):
        steps = jax.random.uniform(jax.random.fold_in(jax.random.fold_in(rng, 6), dim), (shards_of,), jnp.float32, smallest / len(cuts), top_value / len(cuts))
        return jnp.repeat(jnp.exp(steps), extent[dim] // shards_of).reshape((-1,) + (1,) * (len(extent) - dim - 1))

    gain = one(*cuts[0])
    for cut in cuts[1:]:
        gain = gain * one(*cut)
    return gain


def scatter_about(stream_key, extent, width, limit, pieces=(), kind=jnp.bfloat16):
    loudness = block_scale(stream_key, extent, pieces, -0.22, 0.18) if pieces else 1.0
    values = jax.random.normal(stream_key, extent, jnp.float32) * width * loudness
    return jnp.minimum(jnp.maximum(values, -limit), limit).astype(kind)


def setup_inputs(seed: int = 0, part: int = 0) -> dict:
    key_of = jax.random.split(jax.random.key(seed), 15)
    part_keys = jax.random.split(jax.random.fold_in(key_of[14], part), 15)
    return {
        "tokens": draw_tokens(jax.random.fold_in(jax.random.fold_in(key_of[14], part), 71), part),
        "attn_gain": jnp.clip(1.0 + 0.18 * jax.random.normal(key_of[1], (D,), jnp.float32), 0.099609375, 1.8984375).astype(jnp.bfloat16),
        "query_weight": scatter_about(key_of[2], (D, QUERY_HEADS * HEAD_DIM), D ** -0.5, 0.09375, ((0, 4), (1, 4))),
        "key_weight": scatter_about(key_of[3], (KV_HEADS * HEAD_DIM, D), D ** -0.5, 0.09375, ((0, 4), (1, 4))),
        "value_weight": scatter_about(key_of[4], (KV_HEADS * HEAD_DIM, D), D ** -0.5, 0.09375, ((0, 4), (1, 4))),
        "forget_weight": scatter_about(key_of[5], (QUERY_HEADS, D), D ** -0.5, 0.09375, ((1, 4),)),
        "forget_bias": jnp.clip(jax.random.uniform(key_of[6], (QUERY_HEADS,), jnp.float32, -3.0, 1.0), -3.0, 1.0),
        "cache_keys": draw_cache_keys(jax.random.fold_in(jax.random.fold_in(key_of[14], part), 71), part),
        "cache_values": scatter_about(part_keys[8], (BATCH_SEQUENCES, KV_HEADS, HEAD_DIM, CACHE_POSITIONS), 1.0, 6.0, ((1, 4), (3, 4))),
        "gate_sums": draw_gate_sums(jax.random.fold_in(jax.random.fold_in(key_of[14], part), 71), part),
        "output_weight": scatter_about(key_of[10], (QUERY_HEADS * HEAD_DIM, D), (QUERY_HEADS * HEAD_DIM) ** -0.5, 0.09375, ((0, 4), (1, 4))),
        "mixer_gain": jnp.clip(1.0 + 0.18 * jax.random.normal(key_of[11], (D,), jnp.float32), 0.099609375, 1.8984375).astype(jnp.bfloat16),
        "up_weight": scatter_about(key_of[12], (D, FF), D ** -0.5, 0.09375, ((0, 4), (1, 4))),
        "down_weight": scatter_about(key_of[13], (FF, D), FF ** -0.5, 0.046875, ((0, 4), (1, 4))),
    }


epsilon = 1e-06

def row_projection(scaled, weight):
    return lax.dot_general(scaled, weight, (((1,), (1,)), ((), ())), preferred_element_type=jnp.float32)

def reference(tokens, attn_gain, query_weight, key_weight, value_weight, forget_weight, forget_bias, cache_keys, cache_values, gate_sums, output_weight, mixer_gain, up_weight, down_weight):
    head_group = QUERY_HEADS // KV_HEADS
    inverse_root = 1.0 / math.sqrt(HEAD_DIM)
    wide_tokens = tokens.astype(jnp.float32)
    row_scale = lax.rsqrt(lax.optimization_barrier(jnp.mean(wide_tokens * wide_tokens, axis=1, keepdims=True)) + epsilon)
    scaled = (wide_tokens * attn_gain.astype(jnp.float32)).astype(jnp.bfloat16)
    query_vectors = (row_scale * jnp.dot(scaled, query_weight, preferred_element_type=jnp.float32)).astype(jnp.bfloat16)
    fresh_key_rows = (row_scale * row_projection(scaled, key_weight)).astype(jnp.bfloat16)
    new_values = (row_scale * row_projection(scaled, value_weight)).astype(jnp.bfloat16)
    new_gates = jax.nn.log_sigmoid(row_scale * row_projection(scaled, forget_weight) + forget_bias[None, :])

    def attend_one(packed):
        query_row, key_row, value_row, gate_row, key_entries, values, sums = packed
        grouped = query_row.astype(jnp.float32).reshape(KV_HEADS, head_group, HEAD_DIM)
        scores = jnp.einsum('kgd,kdp->kgp', grouped, key_entries.astype(jnp.float32)) * inverse_root
        scores = scores + sums.reshape(KV_HEADS, head_group, -1) + gate_row.reshape(KV_HEADS, head_group, 1)
        own_score = jnp.einsum('kgd,kd->kg', grouped, key_row.astype(jnp.float32).reshape(KV_HEADS, HEAD_DIM)) * inverse_root
        highest = jnp.maximum(lax.optimization_barrier(jnp.max(scores, axis=2)), own_score)
        weights = jnp.exp(scores - highest[..., None])
        own_weight = jnp.exp(own_score - highest)
        totals = lax.optimization_barrier(jnp.sum(weights, axis=2)) + own_weight
        weighted = jnp.einsum('kgp,kdp->kgd', weights, values.astype(jnp.float32), precision=lax.Precision.HIGHEST)
        weighted = weighted + own_weight[..., None] * value_row.astype(jnp.float32).reshape(KV_HEADS, 1, HEAD_DIM)
        return (weighted / totals[..., None]).reshape(QUERY_HEADS * HEAD_DIM).astype(jnp.bfloat16)
    attended = lax.map(attend_one, (query_vectors, fresh_key_rows, new_values, new_gates, cache_keys, cache_values, gate_sums))
    attn_out = jnp.dot(attended, output_weight, preferred_element_type=jnp.float32)
    hidden = (wide_tokens + attn_out).astype(jnp.bfloat16)
    wide_hidden = hidden.astype(jnp.float32)
    mixer_scale = lax.rsqrt(lax.optimization_barrier(jnp.mean(wide_hidden * wide_hidden, axis=1, keepdims=True)) + epsilon)
    scaled_mixer = (wide_hidden * mixer_gain.astype(jnp.float32)).astype(jnp.bfloat16)
    upward = mixer_scale * jnp.dot(scaled_mixer, up_weight, preferred_element_type=jnp.float32)
    active = jnp.square(jax.nn.relu(upward)).astype(jnp.bfloat16)
    return (wide_hidden + jnp.dot(active, down_weight, preferred_element_type=jnp.float32)).astype(jnp.bfloat16)
```

```python
import functools
import math

import jax
import jax.numpy as jnp
from jax import lax
from jax.experimental import pallas as pl
from jax.experimental.pallas import tpu as pltpu
from jax.sharding import PartitionSpec as P

D = 4096
HEAD_DIM = 64


epsilon = 1e-06


def joined(value, axis, join):
    pieces = jax.tree.map(lambda part: lax.all_gather(part, axis), value)
    head = jax.tree.map(lambda part: part[0], pieces)
    tail = jax.tree.map(lambda part: part[1:], pieces)
    running, _ = lax.scan(lambda running, share: (join(running, share), None), head, tail)
    return running


def position_sums(values):
    return lax.psum(values, "kv")


def combine_parts(former, latter):
    highest = jnp.maximum(former[0], latter[0])
    former_scale = jnp.exp(former[0] - highest)
    latter_scale = jnp.exp(latter[0] - highest)
    totals = former[1] * former_scale + latter[1] * latter_scale
    weighted = former[2] * former_scale[..., None] + latter[2] * latter_scale[..., None]
    return (highest, totals, weighted)


def row_projection(scaled, weight):
    return lax.dot_general(
        scaled, weight, (((1,), (1,)), ((), ())), preferred_element_type=jnp.float32
    )


def square_relu(upward, squares):
    mixer_scale = lax.rsqrt(squares / D + epsilon)[:, None]
    return jnp.square(jax.nn.relu(mixer_scale * upward)).astype(jnp.bfloat16)


def per_device(
    tokens,
    attn_gain,
    query_weight,
    key_weight,
    value_weight,
    forget_weight,
    forget_bias,
    cache_keys,
    cache_values,
    gate_sums,
    output_weight,
    mixer_gain,
    up_weight,
    down_weight,
):
    batch_rows = tokens.shape[0]
    own_width = tokens.shape[1]
    key_heads = cache_keys.shape[1]
    local_heads = gate_sums.shape[1]
    head_group = local_heads // key_heads
    inverse_root = 1.0 / math.sqrt(HEAD_DIM)
    row_block = lax.all_gather(tokens, "tp", axis=1, tiled=True)
    wide_block = row_block.astype(jnp.float32)
    squares = jnp.sum(wide_block * wide_block, axis=1)
    scaled = (wide_block * attn_gain.astype(jnp.float32)).astype(jnp.bfloat16)
    part_query = jnp.dot(scaled, query_weight, preferred_element_type=jnp.float32)
    part_key = row_projection(scaled, key_weight)
    part_value = row_projection(scaled, value_weight)
    part_gate = row_projection(scaled, forget_weight)
    squares = position_sums(squares)
    part_query, part_key, part_value, part_gate = position_sums(
        (part_query, part_key, part_value, part_gate)
    )
    row_scale = lax.rsqrt(squares / D + epsilon)[:, None]
    query_vectors = (
        (row_scale * part_query)
        .astype(jnp.bfloat16)
        .reshape(batch_rows, key_heads, head_group, HEAD_DIM)
    )
    fresh_key_rows = (
        (row_scale * part_key).astype(jnp.bfloat16).reshape(batch_rows, key_heads, HEAD_DIM)
    )
    new_values = (
        (row_scale * part_value).astype(jnp.bfloat16).reshape(batch_rows, key_heads, 1, HEAD_DIM)
    )
    gate_input = lax.dynamic_slice_in_dim(
        row_scale * part_gate + forget_bias[None, :],
        lax.axis_index("tp") * local_heads,
        local_heads,
        1,
    )
    new_gates = jax.nn.log_sigmoid(gate_input).reshape(batch_rows, key_heads, head_group)
    scores = (
        jnp.einsum("bkgd,bkdp->bkgp", query_vectors, cache_keys, preferred_element_type=jnp.float32)
        * inverse_root
    )
    scores = (
        scores + gate_sums.reshape(batch_rows, key_heads, head_group, -1) + new_gates[..., None]
    )
    own_score = (
        jnp.einsum(
            "jwcs,jws->jwc", query_vectors, fresh_key_rows, preferred_element_type=jnp.float32
        )
        * inverse_root
    )
    is_last = lax.axis_index("kv") == lax.axis_size("kv") - 1
    own_score = jnp.where(is_last, own_score, -jnp.inf)
    highest = jnp.maximum(jnp.max(scores, axis=3), own_score)
    weights = jnp.exp(scores - highest[..., None])
    own_weight = jnp.exp(own_score - highest)
    totals = jnp.sum(weights, axis=3) + own_weight
    weighted = jnp.einsum(
        "bkgp,bkdp->bkgd",
        weights,
        cache_values.astype(jnp.float32),
        precision=lax.Precision.HIGHEST,
    )
    weighted = weighted + own_weight[..., None] * new_values.astype(jnp.float32)
    highest, totals, weighted = joined((highest, totals, weighted), "kv", combine_parts)
    attended = (
        (weighted / totals[..., None])
        .astype(jnp.bfloat16)
        .reshape(batch_rows, local_heads * HEAD_DIM)
    )
    attn_part = jnp.dot(attended, output_weight, preferred_element_type=jnp.float32)
    attn_out = lax.psum(attn_part, "tp")
    hidden = (wide_block + attn_out).astype(jnp.bfloat16)
    wide_hidden = hidden.astype(jnp.float32)
    squares_mixer = jnp.sum(wide_hidden * wide_hidden, axis=1)
    scaled_mixer = (wide_hidden * mixer_gain.astype(jnp.float32)).astype(jnp.bfloat16)
    part_up = jnp.dot(scaled_mixer, up_weight, preferred_element_type=jnp.float32)
    squares_mixer = position_sums(squares_mixer)
    up_share = lax.psum_scatter(part_up, "kv", scatter_dimension=1, tiled=True)
    active_share = square_relu(up_share, squares_mixer)
    active = lax.all_gather(active_share, "kv", axis=1, tiled=True)
    down_part = jnp.dot(active, down_weight, preferred_element_type=jnp.float32)
    down_share = lax.psum_scatter(down_part, "tp", scatter_dimension=1, tiled=True)
    own_hidden = lax.dynamic_slice_in_dim(hidden, lax.axis_index("tp") * own_width, own_width, 1)
    return (own_hidden.astype(jnp.float32) + down_share).astype(jnp.bfloat16)


F32 = jnp.float32
BF16 = jnp.bfloat16


def nt_dot(left, right):
    return lax.dot_general(left, right, (((1,), (1,)), ((), ())), preferred_element_type=F32)


def nn_dot(left, right):
    return jnp.dot(left, right, preferred_element_type=F32)


def iota(shape, dim):
    return lax.broadcasted_iota(jnp.int32, shape, dim)


def layer_kernel(
    n_kv,
    n_tp,
    width,
    tok_ref,
    again_ref,
    mgain_ref,
    bias_ref,
    wq_hbm,
    wk_hbm,
    wv_hbm,
    wf_hbm,
    ck_hbm,
    cv_hbm,
    gs_hbm,
    wo_hbm,
    up_hbm,
    down_hbm,
    out_ref,
    wq,
    wk,
    wv,
    wf,
    ck,
    cv,
    gs,
    wo,
    up,
    down,
    local_sem,
    up_sem,
    down_sem,
    tokb,
    proj_out,
    proj_in,
    small_out,
    small_in,
    part_out,
    part_in,
    lse_out,
    lse_in,
    attn_out,
    attn_in,
    sq_out,
    sq_in,
    up_out,
    up_in,
    act,
    dn_out,
    dn_in,
    hid,
    fold,
    ob,
    send_kv,
    recv_kv,
    send_tp,
    recv_tp,
):
    kv = lax.axis_index("kv")
    tp = lax.axis_index("tp")
    rows, own = tok_ref.shape
    block = own * n_tp
    inner = wq.shape[1]
    key_width = wk.shape[0]
    heads = gs.shape[1]
    dim = inner // heads
    key_heads = key_width // dim
    group = heads // key_heads
    all_heads = wf.shape[0]
    unit = up.shape[2]
    inverse_root = 1.0 / math.sqrt(dim)

    sources = (
        (wq_hbm, wq),
        (wk_hbm, wk),
        (wv_hbm, wv),
        (wf_hbm, wf),
        (ck_hbm, ck),
        (gs_hbm, gs),
        (cv_hbm, cv),
        (wo_hbm, wo),
    )
    loads = []
    for i, (hbm, vmem) in enumerate(sources):
        loads.append(pltpu.make_async_copy(hbm, vmem, local_sem.at[i]))
    up_loads = []
    down_loads = []
    for off in range(n_kv):
        target = lax.rem(kv + off, n_kv)
        up_loads.append(
            pltpu.make_async_copy(
                up_hbm.at[:, pl.ds(pl.multiple_of(target * unit, unit), unit)],
                up.at[off],
                up_sem.at[off],
            )
        )
        origin = lax.rem(kv - off + n_kv, n_kv)
        down_loads.append(
            pltpu.make_async_copy(
                down_hbm.at[pl.ds(pl.multiple_of(origin * unit, unit), unit), :],
                down.at[off],
                down_sem.at[off],
            )
        )
    own_tok = pltpu.make_async_copy(tok_ref, tokb.at[tp], local_sem.at[len(sources)])
    own_tok.start()
    for load in loads:
        load.start()
    for off in list(range(1, n_kv)) + [0]:
        up_loads[off].start()
    for off in range(n_kv):
        down_loads[off].start()

    barrier = pltpu.get_barrier_semaphore()
    for off in range(1, n_tp):
        pl.semaphore_signal(
            barrier,
            inc=1,
            device_id={"tp": lax.rem(tp + off, n_tp)},
            device_id_type=pl.DeviceIdType.MESH,
        )
    for off in range(1, n_kv):
        pl.semaphore_signal(
            barrier,
            inc=1,
            device_id={"kv": lax.rem(kv + off, n_kv)},
            device_id_type=pl.DeviceIdType.MESH,
        )
    pl.semaphore_wait(barrier, n_tp + n_kv - 2)

    sent = []

    def send(axis, phase, off, source, target):
        me, n = (kv, n_kv) if axis == "kv" else (tp, n_tp)
        sends, recvs = (send_kv, recv_kv) if axis == "kv" else (send_tp, recv_tp)
        copy = pltpu.make_async_remote_copy(
            src_ref=source,
            dst_ref=target,
            send_sem=sends.at[phase, off],
            recv_sem=recvs.at[phase, off],
            device_id={axis: lax.rem(me + off, n)},
            device_id_type=pl.DeviceIdType.MESH,
        )
        copy.start()
        sent.append(copy)
        return copy

    tok_copies = [send("tp", 0, off, tok_ref, tokb.at[tp]) for off in range(1, n_tp)]

    lane = iota((heads, inner), 1)
    spread = (lane // dim) == iota((heads, inner), 0)
    fold_row, fold_lane = iota((inner, key_width), 0), iota((inner, key_width), 1)
    fold[...] = jnp.where(
        (fold_row // (dim * group) == fold_lane // dim) & (fold_row % dim == fold_lane % dim),
        1.0,
        0.0,
    ).astype(BF16)
    head_of = jnp.where(iota((128, inner), 1) // dim == iota((128, inner), 0), 1.0, 0.0).astype(BF16)
    lse_out[...] = jnp.zeros_like(lse_out)
    key_mask = (iota((heads, key_width), 1) // dim) == (iota((heads, key_width), 0) // group)
    slim_lane = iota((heads, 128), 1)
    slim_row = iota((heads, 128), 0)

    own_tok.wait()
    for copy in tok_copies:
        copy.wait_recv()
    wide = jnp.concatenate([tokb[j].astype(F32) for j in range(n_tp)], axis=1)
    squares = jnp.sum(wide * wide, axis=1, keepdims=True)
    scaled = (wide * again_ref[...].astype(F32)).astype(BF16)
    for load in loads[:4]:
        load.wait()
    part_qkv = jnp.concatenate(
        [nn_dot(scaled, wq[...]), nt_dot(scaled, wk[...]), nt_dot(scaled, wv[...])], axis=1
    )
    proj_out[0:rows, :] = part_qkv.astype(BF16)
    part_gate = jnp.concatenate(
        [
            nt_dot(scaled, wf[...]),
            jnp.broadcast_to(squares, (rows, small_out.shape[1] - all_heads)),
        ],
        axis=1,
    )
    small_out[0:rows, :] = part_gate
    proj_copies = []
    for off in range(1, n_kv):
        proj_copies.append(send("kv", 0, off, proj_out, proj_in.at[off]))
        proj_copies.append(send("kv", 1, off, small_out, small_in.at[off]))
    for copy in proj_copies:
        copy.wait_recv()
    for off in range(1, n_kv):
        part_qkv = part_qkv + proj_in[off, 0:rows, :].astype(F32)
        part_gate = part_gate + small_in[off, 0:rows, :]
    row_scale = lax.rsqrt(part_gate[:, all_heads : all_heads + 1] / width + epsilon)
    qkv = row_scale * part_qkv
    queries = qkv[:, :inner].astype(BF16).astype(F32)
    new_keys = qkv[:, inner : inner + key_width].astype(BF16).astype(F32)
    new_values = qkv[:, inner + key_width :].astype(BF16).astype(F32)
    gate_in = row_scale * part_gate + bias_ref[...]
    gates = jnp.minimum(gate_in, 0.0) - jnp.log1p(jnp.exp(-jnp.abs(gate_in)))
    folded = []
    diagonal = jnp.concatenate(
        [
            jnp.where(spread, jnp.broadcast_to(queries[b : b + 1, :], (heads, inner)), 0.0).astype(BF16)
            for b in range(rows)
        ],
        axis=0,
    )
    folded = nn_dot(diagonal, fold[...])
    is_last = iota((heads, 1), 0) * 0 + kv == n_kv - 1
    for load in loads[4:7]:
        load.wait()
    for b in range(rows):
        query = folded[b * heads : (b + 1) * heads, :]
        gate = jnp.sum(
            jnp.where(slim_lane == slim_row + tp * heads, gates[b : b + 1, :], 0.0),
            axis=1,
            keepdims=True,
        )
        scores = nn_dot(query.astype(BF16), ck[b]) * inverse_root + gs[b] + gate
        own_score = (
            jnp.sum(query * new_keys[b : b + 1, :], axis=1, keepdims=True) * inverse_root
        )
        own_score = jnp.where(is_last, own_score, -jnp.inf)
        highest = jnp.maximum(jnp.max(scores, axis=1, keepdims=True), own_score)
        weights = jnp.exp(scores - highest)
        own_weight = jnp.exp(own_score - highest)
        totals = jnp.sum(weights, axis=1, keepdims=True) + own_weight
        weighted = nt_dot(weights.astype(BF16), cv[b]) + own_weight * new_values[b : b + 1, :]
        ob[b * heads : (b + 1) * heads, :] = jnp.where(key_mask, weighted / totals, 0.0).astype(BF16)
        lse = highest + jnp.log(totals)
        lse_out[b : b + 1, :] = jnp.sum(
            jnp.where(slim_lane == slim_row, lse, 0.0), axis=0, keepdims=True
        )
    lse_copies = [send("kv", 2, off, lse_out, lse_in.at[off]) for off in range(1, n_kv)]
    unfolded = nt_dot(ob[...], fold[...])
    part = jnp.concatenate(
        [
            jnp.sum(
                jnp.where(spread, unfolded[b * heads : (b + 1) * heads, :], 0.0),
                axis=0,
                keepdims=True,
            )
            for b in range(rows)
        ],
        axis=0,
    )
    part_out[0:rows, :] = part.astype(BF16)
    lse_copies += [send("kv", 3, off, part_out, part_in.at[off]) for off in range(1, n_kv)]
    for copy in lse_copies:
        copy.wait_recv()
    logs = [lse_out[...]] + [lse_in[off] for off in range(1, n_kv)]
    top = functools.reduce(jnp.maximum, logs)
    shares = [jnp.exp(log - top) for log in logs]
    whole = functools.reduce(jnp.add, shares)
    pieces = []
    for share in shares:
        share = share / whole
        high = share.astype(BF16).astype(F32)
        pieces += [high, share - high]
    expanded = nn_dot(jnp.concatenate(pieces, axis=0).astype(BF16), head_of)
    padded = lse_out.shape[0]
    attended = jnp.zeros((rows, inner), F32)
    for off in range(n_kv):
        at = 2 * off * padded
        share = expanded[at : at + rows] + expanded[at + padded : at + padded + rows]
        block_part = part if off == 0 else part_in[off, 0:rows, :].astype(F32)
        attended = attended + share * block_part
    loads[7].wait()
    attn = nn_dot(attended.astype(BF16), wo[...])
    attn_out[0:rows, :] = attn.astype(BF16)
    attn_copies = [send("tp", 1, off, attn_out, attn_in.at[off]) for off in range(1, n_tp)]
    for copy in attn_copies:
        copy.wait_recv()
    for off in range(1, n_tp):
        attn = attn + attn_in[off, 0:rows, :].astype(F32)
    hidden = (wide + attn).astype(BF16).astype(F32)
    squares_mixer = jnp.sum(hidden * hidden, axis=1, keepdims=True)
    sq_out[0:rows, :] = jnp.broadcast_to(squares_mixer, (rows, sq_out.shape[1]))
    up_copies = [send("kv", 4, off, sq_out, sq_in.at[off]) for off in range(1, n_kv)]
    for j in range(n_tp):
        hid[j, 0:rows, :] = hidden[:, j * own : (j + 1) * own]
    scaled_mixer = (hidden * mgain_ref[...].astype(F32)).astype(BF16)
    for off in range(1, n_kv):
        up_loads[off].wait()
        up_out[off, 0:rows, :] = nn_dot(scaled_mixer, up[off]).astype(BF16)
        up_copies.append(send("kv", 5, off, up_out.at[off], up_in.at[off]))
    up_loads[0].wait()
    upward = nn_dot(scaled_mixer, up[0])
    for copy in up_copies:
        copy.wait_recv()
    for off in range(1, n_kv):
        upward = upward + up_in[off, 0:rows, :].astype(F32)
        squares_mixer = squares_mixer + sq_in[off, 0:rows, 0:1]
    mixer_scale = lax.rsqrt(squares_mixer / width + epsilon)
    upward = jnp.maximum(mixer_scale * upward, 0.0)
    active = (upward * upward).astype(BF16)
    act[0, 0:rows, :] = active
    act_copies = [send("kv", 6, off, act.at[0], act.at[off]) for off in range(1, n_kv)]
    down_loads[0].wait()
    mixed = nn_dot(active, down[0])
    for off in range(1, n_kv):
        down_loads[off].wait()
        act_copies[off - 1].wait_recv()
        mixed = mixed + nn_dot(act[off, 0:rows, :], down[off])
    for j in range(n_tp):
        dn_out[j, 0:rows, :] = mixed[:, j * own : (j + 1) * own].astype(BF16)
        hid[j, 0:rows, :] = hid[j, 0:rows, :] + mixed[:, j * own : (j + 1) * own]
    dn_copies = []
    for off in range(1, n_tp):
        target = lax.rem(tp + off, n_tp)
        dn_copies.append(send("tp", 2, off, dn_out.at[target], dn_in.at[off]))
    result = hid[tp, 0:rows, :]
    for copy in dn_copies:
        copy.wait_recv()
    for off in range(1, n_tp):
        result = result + dn_in[off, 0:rows, :].astype(F32)
    out_ref[...] = result.astype(BF16)
    for copy in sent:
        copy.wait_send()


def fused_device(n_kv, n_tp, *arrays):
    (tokens, attn_gain, wq, wk, wv, wf, bias, ck, cv, gs, wo, mixer_gain, up, down) = arrays
    rows, own = tokens.shape
    batch, key_heads, dim, positions = ck.shape
    flat = (batch, key_heads * dim, positions)
    unit = up.shape[1] // n_kv
    inner = wq.shape[1]
    key_width = wk.shape[0]
    heads = gs.shape[1]
    block = wq.shape[0]
    padded = -(-rows // 16) * 16
    slim = -(-(wf.shape[0] + 1) // 128) * 128
    bias_row = jnp.pad(bias[None, :], ((0, 0), (0, slim - bias.shape[0])))
    vmem = pltpu.VMEM
    scratch = [
        vmem(wq.shape, BF16),
        vmem(wk.shape, BF16),
        vmem(wv.shape, BF16),
        vmem(wf.shape, BF16),
        vmem(flat, BF16),
        vmem(flat, BF16),
        vmem(gs.shape, F32),
        vmem(wo.shape, BF16),
        vmem((n_kv, up.shape[0], unit), BF16),
        vmem((n_kv, unit, down.shape[1]), BF16),
        pltpu.SemaphoreType.DMA((9,)),
        pltpu.SemaphoreType.DMA((n_kv,)),
        pltpu.SemaphoreType.DMA((n_kv,)),
        vmem((n_tp, rows, own), BF16),
        vmem((padded, inner + 2 * key_width), BF16),
        vmem((n_kv, padded, inner + 2 * key_width), BF16),
        vmem((padded, slim), F32),
        vmem((n_kv, padded, slim), F32),
        vmem((padded, inner), BF16),
        vmem((n_kv, padded, inner), BF16),
        vmem((padded, 128), F32),
        vmem((n_kv, padded, 128), F32),
        vmem((padded, block), BF16),
        vmem((n_tp, padded, block), BF16),
        vmem((padded, 128), F32),
        vmem((n_kv, padded, 128), F32),
        vmem((n_kv, padded, unit), BF16),
        vmem((n_kv, padded, unit), BF16),
        vmem((n_kv, padded, unit), BF16),
        vmem((n_tp, padded, own), BF16),
        vmem((n_tp, padded, own), BF16),
        vmem((n_tp, padded, own), F32),
        vmem((inner, key_width), BF16),
        vmem((rows * heads, key_width), BF16),
        pltpu.SemaphoreType.DMA((7, n_kv)),
        pltpu.SemaphoreType.DMA((7, n_kv)),
        pltpu.SemaphoreType.DMA((3, n_tp)),
        pltpu.SemaphoreType.DMA((3, n_tp)),
    ]
    in_vmem = pl.BlockSpec(memory_space=pltpu.VMEM)
    in_hbm = pl.BlockSpec(memory_space=pl.ANY)
    return pl.pallas_call(
        functools.partial(layer_kernel, n_kv, n_tp, D),
        out_shape=jax.ShapeDtypeStruct((rows, own), BF16),
        in_specs=[in_vmem] * 4 + [in_hbm] * 10,
        out_specs=in_vmem,
        scratch_shapes=scratch,
        compiler_params=pltpu.CompilerParams(
            collective_id=0, has_side_effects=True, vmem_limit_bytes=60 * 1024 * 1024
        ),
    )(
        tokens,
        attn_gain[None, :],
        mixer_gain[None, :],
        bias_row,
        wq,
        wk,
        wv,
        wf,
        ck.reshape(flat),
        cv.reshape(flat),
        gs,
        wo,
        up,
        down,
    )


def solution(mesh):
    n_kv, n_tp = mesh.shape["kv"], mesh.shape["tp"]

    def device(*arrays):
        tokens, wk, up = arrays[0], arrays[3], arrays[12]
        lanes = (tokens.shape[1], wk.shape[0], up.shape[1] // n_kv)
        if any(width % 128 for width in lanes):
            return per_device(*arrays)
        return fused_device(n_kv, n_tp, *arrays)

    placed = (
        P("grp", ("kv", "tp")),
        P("kv"),
        P("kv", "tp"),
        P("tp", "kv"),
        P("tp", "kv"),
        P(None, "kv"),
        P(),
        P("grp", "tp", None, "kv"),
        P("grp", "tp", None, "kv"),
        P("grp", "tp", "kv"),
        P("tp", "kv"),
        P("kv"),
        P("kv", "tp"),
        P("tp", "kv"),
    )
    return jax.shard_map(
        device, mesh=mesh, in_specs=placed, out_specs=P("grp", ("kv", "tp")), check_vma=False
    )
```

```python
import functools
import math

import jax
import jax.numpy as jnp
from jax import lax
from jax.experimental import pallas as pl
from jax.experimental.pallas import tpu as pltpu
from jax.sharding import PartitionSpec as P

D = 4096
HEAD_DIM = 64


epsilon = 1e-06


def joined(value, axis, join):
    pieces = jax.tree.map(lambda part: lax.all_gather(part, axis), value)
    head = jax.tree.map(lambda part: part[0], pieces)
    tail = jax.tree.map(lambda part: part[1:], pieces)
    running, _ = lax.scan(lambda running, share: (join(running, share), None), head, tail)
    return running


def position_sums(values):
    return lax.psum(values, "kv")


def combine_parts(former, latter):
    highest = jnp.maximum(former[0], latter[0])
    former_scale = jnp.exp(former[0] - highest)
    latter_scale = jnp.exp(latter[0] - highest)
    totals = former[1] * former_scale + latter[1] * latter_scale
    weighted = former[2] * former_scale[..., None] + latter[2] * latter_scale[..., None]
    return (highest, totals, weighted)


def row_projection(scaled, weight):
    return lax.dot_general(
        scaled, weight, (((1,), (1,)), ((), ())), preferred_element_type=jnp.float32
    )


def square_relu(upward, squares):
    mixer_scale = lax.rsqrt(squares / D + epsilon)[:, None]
    return jnp.square(jax.nn.relu(mixer_scale * upward)).astype(jnp.bfloat16)


def per_device(
    tokens,
    attn_gain,
    query_weight,
    key_weight,
    value_weight,
    forget_weight,
    forget_bias,
    cache_keys,
    cache_values,
    gate_sums,
    output_weight,
    mixer_gain,
    up_weight,
    down_weight,
):
    batch_rows = tokens.shape[0]
    own_width = tokens.shape[1]
    key_heads = cache_keys.shape[1]
    local_heads = gate_sums.shape[1]
    head_group = local_heads // key_heads
    inverse_root = 1.0 / math.sqrt(HEAD_DIM)
    row_block = lax.all_gather(tokens, "tp", axis=1, tiled=True)
    wide_block = row_block.astype(jnp.float32)
    squares = jnp.sum(wide_block * wide_block, axis=1)
    scaled = (wide_block * attn_gain.astype(jnp.float32)).astype(jnp.bfloat16)
    part_query = jnp.dot(scaled, query_weight, preferred_element_type=jnp.float32)
    part_key = row_projection(scaled, key_weight)
    part_value = row_projection(scaled, value_weight)
    part_gate = row_projection(scaled, forget_weight)
    squares = position_sums(squares)
    part_query, part_key, part_value, part_gate = position_sums(
        (part_query, part_key, part_value, part_gate)
    )
    row_scale = lax.rsqrt(squares / D + epsilon)[:, None]
    query_vectors = (
        (row_scale * part_query)
        .astype(jnp.bfloat16)
        .reshape(batch_rows, key_heads, head_group, HEAD_DIM)
    )
    fresh_key_rows = (
        (row_scale * part_key).astype(jnp.bfloat16).reshape(batch_rows, key_heads, HEAD_DIM)
    )
    new_values = (
        (row_scale * part_value).astype(jnp.bfloat16).reshape(batch_rows, key_heads, 1, HEAD_DIM)
    )
    gate_input = lax.dynamic_slice_in_dim(
        row_scale * part_gate + forget_bias[None, :],
        lax.axis_index("tp") * local_heads,
        local_heads,
        1,
    )
    new_gates = jax.nn.log_sigmoid(gate_input).reshape(batch_rows, key_heads, head_group)
    scores = (
        jnp.einsum("bkgd,bkdp->bkgp", query_vectors, cache_keys, preferred_element_type=jnp.float32)
        * inverse_root
    )
    scores = (
        scores + gate_sums.reshape(batch_rows, key_heads, head_group, -1) + new_gates[..., None]
    )
    own_score = (
        jnp.einsum(
            "jwcs,jws->jwc", query_vectors, fresh_key_rows, preferred_element_type=jnp.float32
        )
        * inverse_root
    )
    is_last = lax.axis_index("kv") == lax.axis_size("kv") - 1
    own_score = jnp.where(is_last, own_score, -jnp.inf)
    highest = jnp.maximum(jnp.max(scores, axis=3), own_score)
    weights = jnp.exp(scores - highest[..., None])
    own_weight = jnp.exp(own_score - highest)
    totals = jnp.sum(weights, axis=3) + own_weight
    weighted = jnp.einsum(
        "bkgp,bkdp->bkgd",
        weights,
        cache_values.astype(jnp.float32),
        precision=lax.Precision.HIGHEST,
    )
    weighted = weighted + own_weight[..., None] * new_values.astype(jnp.float32)
    highest, totals, weighted = joined((highest, totals, weighted), "kv", combine_parts)
    attended = (
        (weighted / totals[..., None])
        .astype(jnp.bfloat16)
        .reshape(batch_rows, local_heads * HEAD_DIM)
    )
    attn_part = jnp.dot(attended, output_weight, preferred_element_type=jnp.float32)
    attn_out = lax.psum(attn_part, "tp")
    hidden = (wide_block + attn_out).astype(jnp.bfloat16)
    wide_hidden = hidden.astype(jnp.float32)
    squares_mixer = jnp.sum(wide_hidden * wide_hidden, axis=1)
    scaled_mixer = (wide_hidden * mixer_gain.astype(jnp.float32)).astype(jnp.bfloat16)
    part_up = jnp.dot(scaled_mixer, up_weight, preferred_element_type=jnp.float32)
    squares_mixer = position_sums(squares_mixer)
    up_share = lax.psum_scatter(part_up, "kv", scatter_dimension=1, tiled=True)
    active_share = square_relu(up_share, squares_mixer)
    active = lax.all_gather(active_share, "kv", axis=1, tiled=True)
    down_part = jnp.dot(active, down_weight, preferred_element_type=jnp.float32)
    down_share = lax.psum_scatter(down_part, "tp", scatter_dimension=1, tiled=True)
    own_hidden = lax.dynamic_slice_in_dim(hidden, lax.axis_index("tp") * own_width, own_width, 1)
    return (own_hidden.astype(jnp.float32) + down_share).astype(jnp.bfloat16)


F32 = jnp.float32
BF16 = jnp.bfloat16


def nt_dot(left, right):
    return lax.dot_general(left, right, (((1,), (1,)), ((), ())), preferred_element_type=F32)


def nn_dot(left, right):
    return jnp.dot(left, right, preferred_element_type=F32)


def iota(shape, dim):
    return lax.broadcasted_iota(jnp.int32, shape, dim)


def layer_kernel(
    n_kv,
    n_tp,
    width,
    tok_ref,
    again_ref,
    mgain_ref,
    bias_ref,
    wq_hbm,
    wk_hbm,
    wv_hbm,
    wf_hbm,
    ck_hbm,
    cv_hbm,
    gs_hbm,
    wo_hbm,
    up_hbm,
    down_hbm,
    out_ref,
    wq,
    wk,
    wv,
    wf,
    ck,
    cv,
    gs,
    wo,
    up,
    down,
    local_sem,
    up_sem,
    down_sem,
    tokb,
    proj_out,
    proj_in,
    small_out,
    small_in,
    part_out,
    part_in,
    lse_out,
    lse_in,
    attn_out,
    attn_in,
    sq_out,
    sq_in,
    up_out,
    up_in,
    act,
    dn_out,
    dn_in,
    hid,
    fold,
    ob,
    send_kv,
    recv_kv,
    send_tp,
    recv_tp,
):
    kv = lax.axis_index("kv")
    tp = lax.axis_index("tp")
    rows, own = tok_ref.shape
    block = own * n_tp
    inner = wq.shape[1]
    key_width = wk.shape[0]
    heads = gs.shape[1]
    dim = inner // heads
    key_heads = key_width // dim
    group = heads // key_heads
    all_heads = wf.shape[0]
    unit = up.shape[2]
    inverse_root = 1.0 / math.sqrt(dim)

    sources = (
        (wq_hbm, wq),
        (wk_hbm, wk),
        (wv_hbm, wv),
        (wf_hbm, wf),
        (ck_hbm, ck),
        (gs_hbm, gs),
        (cv_hbm, cv),
        (wo_hbm, wo),
    )
    loads = []
    for i, (hbm, vmem) in enumerate(sources):
        loads.append(pltpu.make_async_copy(hbm, vmem, local_sem.at[i]))
    up_loads = []
    down_loads = []
    for off in range(n_kv):
        target = lax.rem(kv + off, n_kv)
        up_loads.append(
            pltpu.make_async_copy(
                up_hbm.at[:, pl.ds(pl.multiple_of(target * unit, unit), unit)],
                up.at[off],
                up_sem.at[off],
            )
        )
        origin = lax.rem(kv - off + n_kv, n_kv)
        down_loads.append(
            pltpu.make_async_copy(
                down_hbm.at[pl.ds(pl.multiple_of(origin * unit, unit), unit), :],
                down.at[off],
                down_sem.at[off],
            )
        )
    own_tok = pltpu.make_async_copy(tok_ref, tokb.at[tp], local_sem.at[len(sources)])
    own_tok.start()
    for load in loads[:4]:
        load.start()

    barrier = pltpu.get_barrier_semaphore()
    for off in range(1, n_tp):
        pl.semaphore_signal(
            barrier,
            inc=1,
            device_id={"tp": lax.rem(tp + off, n_tp)},
            device_id_type=pl.DeviceIdType.MESH,
        )
    for off in range(1, n_kv):
        pl.semaphore_signal(
            barrier,
            inc=1,
            device_id={"kv": lax.rem(kv + off, n_kv)},
            device_id_type=pl.DeviceIdType.MESH,
        )
    pl.semaphore_wait(barrier, n_tp + n_kv - 2)

    sent = []

    def send(axis, phase, off, source, target):
        me, n = (kv, n_kv) if axis == "kv" else (tp, n_tp)
        sends, recvs = (send_kv, recv_kv) if axis == "kv" else (send_tp, recv_tp)
        copy = pltpu.make_async_remote_copy(
            src_ref=source,
            dst_ref=target,
            send_sem=sends.at[phase, off],
            recv_sem=recvs.at[phase, off],
            device_id={axis: lax.rem(me + off, n)},
            device_id_type=pl.DeviceIdType.MESH,
        )
        copy.start()
        sent.append(copy)
        return copy

    tok_copies = [send("tp", 0, off, tok_ref, tokb.at[tp]) for off in range(1, n_tp)]

    for load in loads[4:]:
        load.start()

    lane = iota((heads, inner), 1)
    spread = (lane // dim) == iota((heads, inner), 0)
    fold_row, fold_lane = iota((inner, key_width), 0), iota((inner, key_width), 1)
    fold[...] = jnp.where(
        (fold_row // (dim * group) == fold_lane // dim) & (fold_row % dim == fold_lane % dim),
        1.0,
        0.0,
    ).astype(BF16)
    head_of = jnp.where(iota((128, inner), 1) // dim == iota((128, inner), 0), 1.0, 0.0).astype(BF16)
    lse_out[...] = jnp.zeros_like(lse_out)
    key_mask = (iota((heads, key_width), 1) // dim) == (iota((heads, key_width), 0) // group)
    slim_lane = iota((heads, 128), 1)
    slim_row = iota((heads, 128), 0)

    own_tok.wait()
    for copy in tok_copies:
        copy.wait_recv()
    wide = jnp.concatenate([tokb[j].astype(F32) for j in range(n_tp)], axis=1)
    squares = jnp.sum(wide * wide, axis=1, keepdims=True)
    scaled = (wide * again_ref[...].astype(F32).reshape(1, block)).astype(BF16)
    for load in loads[:4]:
        load.wait()
    part_qkv = jnp.concatenate(
        [nn_dot(scaled, wq[...]), nt_dot(scaled, wk[...]), nt_dot(scaled, wv[...])], axis=1
    )
    proj_out[0:rows, :] = part_qkv.astype(BF16)
    part_gate = jnp.concatenate(
        [
            nt_dot(scaled, wf[...]),
            jnp.broadcast_to(squares, (rows, small_out.shape[1] - all_heads)),
        ],
        axis=1,
    )
    small_out[0:rows, :] = part_gate
    proj_copies = []
    for off in range(1, n_kv):
        proj_copies.append(send("kv", 0, off, proj_out, proj_in.at[off]))
        proj_copies.append(send("kv", 1, off, small_out, small_in.at[off]))
    for off in list(range(1, n_kv)) + [0]:
        up_loads[off].start()
    for off in range(n_kv):
        down_loads[off].start()
    for copy in proj_copies:
        copy.wait_recv()
    for off in range(1, n_kv):
        part_qkv = part_qkv + proj_in[off, 0:rows, :].astype(F32)
        part_gate = part_gate + small_in[off, 0:rows, :]
    row_scale = lax.rsqrt(part_gate[:, all_heads : all_heads + 1] / width + epsilon)
    qkv = row_scale * part_qkv
    queries = qkv[:, :inner].astype(BF16).astype(F32)
    new_keys = qkv[:, inner : inner + key_width].astype(BF16).astype(F32)
    new_values = qkv[:, inner + key_width :].astype(BF16).astype(F32)
    bias = bias_ref[...].reshape(1, all_heads)
    bias = jnp.concatenate([bias, jnp.zeros((1, part_gate.shape[1] - all_heads), F32)], axis=1)
    gate_in = row_scale * part_gate + bias
    gates = jnp.minimum(gate_in, 0.0) - jnp.log1p(jnp.exp(-jnp.abs(gate_in)))
    folded = []
    diagonal = jnp.concatenate(
        [
            jnp.where(spread, jnp.broadcast_to(queries[b : b + 1, :], (heads, inner)), 0.0).astype(BF16)
            for b in range(rows)
        ],
        axis=0,
    )
    folded = nn_dot(diagonal, fold[...])
    is_last = iota((heads, 1), 0) * 0 + kv == n_kv - 1
    for load in loads[4:7]:
        load.wait()
    for b in range(rows):
        query = folded[b * heads : (b + 1) * heads, :]
        gate = jnp.sum(
            jnp.where(slim_lane == slim_row + tp * heads, gates[b : b + 1, :], 0.0),
            axis=1,
            keepdims=True,
        )
        scores = nn_dot(query.astype(BF16), ck[b]) * inverse_root + gs[b] + gate
        own_score = (
            jnp.sum(query * new_keys[b : b + 1, :], axis=1, keepdims=True) * inverse_root
        )
        own_score = jnp.where(is_last, own_score, -jnp.inf)
        highest = jnp.maximum(jnp.max(scores, axis=1, keepdims=True), own_score)
        weights = jnp.exp(scores - highest)
        own_weight = jnp.exp(own_score - highest)
        totals = jnp.sum(weights, axis=1, keepdims=True) + own_weight
        weighted = nt_dot(weights.astype(BF16), cv[b]) + own_weight * new_values[b : b + 1, :]
        ob[b * heads : (b + 1) * heads, :] = jnp.where(key_mask, weighted / totals, 0.0).astype(BF16)
        lse = highest + jnp.log(totals)
        lse_out[b : b + 1, :] = jnp.sum(
            jnp.where(slim_lane == slim_row, lse, 0.0), axis=0, keepdims=True
        )
    lse_copies = [send("kv", 2, off, lse_out, lse_in.at[off]) for off in range(1, n_kv)]
    unfolded = nt_dot(ob[...], fold[...])
    part = jnp.concatenate(
        [
            jnp.sum(
                jnp.where(spread, unfolded[b * heads : (b + 1) * heads, :], 0.0),
                axis=0,
                keepdims=True,
            )
            for b in range(rows)
        ],
        axis=0,
    )
    part_out[0:rows, :] = part.astype(BF16)
    lse_copies += [send("kv", 3, off, part_out, part_in.at[off]) for off in range(1, n_kv)]
    for copy in lse_copies:
        copy.wait_recv()
    logs = [lse_out[...]] + [lse_in[off] for off in range(1, n_kv)]
    top = functools.reduce(jnp.maximum, logs)
    shares = [jnp.exp(log - top) for log in logs]
    whole = functools.reduce(jnp.add, shares)
    pieces = []
    for share in shares:
        share = share / whole
        high = share.astype(BF16).astype(F32)
        pieces += [high, share - high]
    expanded = nn_dot(jnp.concatenate(pieces, axis=0).astype(BF16), head_of)
    padded = lse_out.shape[0]
    attended = jnp.zeros((rows, inner), F32)
    for off in range(n_kv):
        at = 2 * off * padded
        share = expanded[at : at + rows] + expanded[at + padded : at + padded + rows]
        block_part = part if off == 0 else part_in[off, 0:rows, :].astype(F32)
        attended = attended + share * block_part
    loads[7].wait()
    attn = nn_dot(attended.astype(BF16), wo[...])
    attn_out[0:rows, :] = attn.astype(BF16)
    attn_copies = [send("tp", 1, off, attn_out, attn_in.at[off]) for off in range(1, n_tp)]
    for copy in attn_copies:
        copy.wait_recv()
    for off in range(1, n_tp):
        attn = attn + attn_in[off, 0:rows, :].astype(F32)
    hidden = (wide + attn).astype(BF16).astype(F32)
    squares_mixer = jnp.sum(hidden * hidden, axis=1, keepdims=True)
    sq_out[0:rows, :] = jnp.broadcast_to(squares_mixer, (rows, sq_out.shape[1]))
    up_copies = [send("kv", 4, off, sq_out, sq_in.at[off]) for off in range(1, n_kv)]
    for j in range(n_tp):
        hid[j, 0:rows, :] = hidden[:, j * own : (j + 1) * own]
    scaled_mixer = (hidden * mgain_ref[...].astype(F32).reshape(1, block)).astype(BF16)
    for off in range(1, n_kv):
        up_loads[off].wait()
        up_out[off, 0:rows, :] = nn_dot(scaled_mixer, up[off]).astype(BF16)
        up_copies.append(send("kv", 5, off, up_out.at[off], up_in.at[off]))
    up_loads[0].wait()
    upward = nn_dot(scaled_mixer, up[0])
    for copy in up_copies:
        copy.wait_recv()
    for off in range(1, n_kv):
        upward = upward + up_in[off, 0:rows, :].astype(F32)
        squares_mixer = squares_mixer + sq_in[off, 0:rows, 0:1]
    mixer_scale = lax.rsqrt(squares_mixer / width + epsilon)
    upward = jnp.maximum(mixer_scale * upward, 0.0)
    active = (upward * upward).astype(BF16)
    act[0, 0:rows, :] = active
    act_copies = [send("kv", 6, off, act.at[0], act.at[off]) for off in range(1, n_kv)]
    down_loads[0].wait()
    mixed = nn_dot(active, down[0])
    for off in range(1, n_kv):
        down_loads[off].wait()
        act_copies[off - 1].wait_recv()
        mixed = mixed + nn_dot(act[off, 0:rows, :], down[off])
    for j in range(n_tp):
        dn_out[j, 0:rows, :] = mixed[:, j * own : (j + 1) * own].astype(BF16)
        hid[j, 0:rows, :] = hid[j, 0:rows, :] + mixed[:, j * own : (j + 1) * own]
    dn_copies = []
    for off in range(1, n_tp):
        target = lax.rem(tp + off, n_tp)
        dn_copies.append(send("tp", 2, off, dn_out.at[target], dn_in.at[off]))
    result = hid[tp, 0:rows, :]
    for copy in dn_copies:
        copy.wait_recv()
    for off in range(1, n_tp):
        result = result + dn_in[off, 0:rows, :].astype(F32)
    out_ref[...] = result.astype(BF16)
    for copy in sent:
        copy.wait_send()


def fused_device(n_kv, n_tp, *arrays):
    (tokens, attn_gain, wq, wk, wv, wf, bias, ck, cv, gs, wo, mixer_gain, up, down) = arrays
    rows, own = tokens.shape
    batch, key_heads, dim, positions = ck.shape
    flat = (batch, key_heads * dim, positions)
    unit = up.shape[1] // n_kv
    inner = wq.shape[1]
    key_width = wk.shape[0]
    heads = gs.shape[1]
    block = wq.shape[0]
    padded = -(-rows // 16) * 16
    slim = -(-(wf.shape[0] + 1) // 128) * 128
    vmem = pltpu.VMEM
    scratch = [
        vmem(wq.shape, BF16),
        vmem(wk.shape, BF16),
        vmem(wv.shape, BF16),
        vmem(wf.shape, BF16),
        vmem(flat, BF16),
        vmem(flat, BF16),
        vmem(gs.shape, F32),
        vmem(wo.shape, BF16),
        vmem((n_kv, up.shape[0], unit), BF16),
        vmem((n_kv, unit, down.shape[1]), BF16),
        pltpu.SemaphoreType.DMA((9,)),
        pltpu.SemaphoreType.DMA((n_kv,)),
        pltpu.SemaphoreType.DMA((n_kv,)),
        vmem((n_tp, rows, own), BF16),
        vmem((padded, inner + 2 * key_width), BF16),
        vmem((n_kv, padded, inner + 2 * key_width), BF16),
        vmem((padded, slim), F32),
        vmem((n_kv, padded, slim), F32),
        vmem((padded, inner), BF16),
        vmem((n_kv, padded, inner), BF16),
        vmem((padded, 128), F32),
        vmem((n_kv, padded, 128), F32),
        vmem((padded, block), BF16),
        vmem((n_tp, padded, block), BF16),
        vmem((padded, 128), F32),
        vmem((n_kv, padded, 128), F32),
        vmem((n_kv, padded, unit), BF16),
        vmem((n_kv, padded, unit), BF16),
        vmem((n_kv, padded, unit), BF16),
        vmem((n_tp, padded, own), BF16),
        vmem((n_tp, padded, own), BF16),
        vmem((n_tp, padded, own), F32),
        vmem((inner, key_width), BF16),
        vmem((rows * heads, key_width), BF16),
        pltpu.SemaphoreType.DMA((7, n_kv)),
        pltpu.SemaphoreType.DMA((7, n_kv)),
        pltpu.SemaphoreType.DMA((3, n_tp)),
        pltpu.SemaphoreType.DMA((3, n_tp)),
    ]
    in_vmem = pl.BlockSpec(memory_space=pltpu.VMEM)
    in_hbm = pl.BlockSpec(memory_space=pl.ANY)
    return pl.pallas_call(
        functools.partial(layer_kernel, n_kv, n_tp, D),
        out_shape=jax.ShapeDtypeStruct((rows, own), BF16),
        in_specs=[in_vmem] * 4 + [in_hbm] * 10,
        out_specs=in_vmem,
        scratch_shapes=scratch,
        compiler_params=pltpu.CompilerParams(
            collective_id=0, has_side_effects=True, vmem_limit_bytes=60 * 1024 * 1024
        ),
    )(
        tokens,
        attn_gain,
        mixer_gain,
        bias,
        wq,
        wk,
        wv,
        wf,
        ck.reshape(flat),
        cv.reshape(flat),
        gs,
        wo,
        up,
        down,
    )


def solution(mesh):
    n_kv, n_tp = mesh.shape["kv"], mesh.shape["tp"]

    def device(*arrays):
        tokens, wk, up = arrays[0], arrays[3], arrays[12]
        lanes = (tokens.shape[1], wk.shape[0], up.shape[1] // n_kv)
        if any(width % 128 for width in lanes):
            return per_device(*arrays)
        return fused_device(n_kv, n_tp, *arrays)

    placed = (
        P("grp", ("kv", "tp")),
        P("kv"),
        P("kv", "tp"),
        P("tp", "kv"),
        P("tp", "kv"),
        P(None, "kv"),
        P(),
        P("grp", "tp", None, "kv"),
        P("grp", "tp", None, "kv"),
        P("grp", "tp", "kv"),
        P("tp", "kv"),
        P("kv"),
        P("kv", "tp"),
        P("tp", "kv"),
    )
    return jax.shard_map(
        device, mesh=mesh, in_specs=placed, out_specs=P("grp", ("kv", "tp")), check_vma=False
    )
```
